256 devices in a mesh: ep: 64 (over z, x, core), tp: 4 (over y).
Axes of the slice: x: 4, y: 4, z: 8, core: 2. Of those that a mesh axis runs over, the one named last changes fastest.
Arguments:
- queries: bfloat16 [16384, 1024], P('ep', 'tp'), may hold values from -192 to 192
- keys_values: bfloat16 [16384, 512], P('ep', 'tp'), may hold values from -192 to 192
- log_gate_cum: float32 [16, 16384], P('tp'), as said below
- mix_weight: bfloat16 [1024, 2048], P('tp'), may hold values from -0.1875 to 0.1875
- mix_gain: float32 [2048], replicated, may hold values from 0.1 to 1.9
- moe_in: bfloat16 [49152, 2048], P(('ep', 'tp')), may hold values from -6 to 6
- moe_gain: float32 [2048], replicated, may hold values from 0.1 to 1.9
- routes: int32 [49152, 2], P(('ep', 'tp')), may hold values from 0 to 63, all different within a row; in each aligned block of 192 rows (0 to 191, 192 to 383, ...) at most 9 rows name the same one
- route_weight: float32 [49152, 2], P(('ep', 'tp')), may hold values from 0.25 to 2
- expert_gate: bfloat16 [64, 2048, 1024], P('ep', None, 'tp'), may hold values from -0.125 to 0.125
- expert_up: bfloat16 [64, 2048, 1024], P('ep', None, 'tp'), may hold values from -0.125 to 0.125
- expert_down: bfloat16 [64, 1024, 2048], P('ep', 'tp'), may hold values from -0.1875 to 0.1875
Outputs:
- mix_result: bfloat16 [16384, 2048], P(('ep', 'tp'))
- moe_result: bfloat16 [49152, 2048], P(('ep', 'tp'))
The draws below stay inside these ranges and needn't reach their ends.
Inputs may be any that keep to these rules, and one draw needn't show every extreme that they name: `log_gate_cum`: along positions each head's values never rise. `routes`: each row names 2 different experts. Among the rows of one device no expert is named more than 9 times, and in every draw some device names some expert exactly 9 times.
All inputs are finite; a program needn't handle non-finite values.
Results may differ from the reference program's by a relative error of at most 0.013.
Values may be sent and summed in bfloat16 or wider, within the bound.
A program may use at most 128 MiB of HBM per device.

```python
import math
import jax
import jax.numpy as jnp
import numpy as np
from jax import lax

D = 2048
ASKING_ATTENDERS = 16
KV_HEADS = 4
HEAD = 64
FF = 1024
TOPK = 2
TOK_EP = 256
TOK_M = 192
CONTEXT_SPAN = 16384
EXPERTS = 64
CAP = 9
TOKENS_M = 49152
N_EP = 64
N_TP = 4


def attention_pair(key):
    queries = jnp.clip(jax.random.normal(jax.random.fold_in(key, 31), (CONTEXT_SPAN, ASKING_ATTENDERS * HEAD), jnp.float32), -4.5, 4.5)
    paired = jnp.clip(jax.random.normal(jax.random.fold_in(key, 32), (CONTEXT_SPAN, KV_HEADS, 2, HEAD), jnp.float32), -4.5, 4.5)
    return (queries, paired.reshape(CONTEXT_SPAN, KV_HEADS * 2 * HEAD))


def draw_queries(key, part):
    return attention_pair(key)[0].astype(jnp.bfloat16)


def draw_keys_values(key, part):
    return attention_pair(key)[1].astype(jnp.bfloat16)


def draw_log_gate_cum(key, part):
    attender_ordinal = jnp.arange(ASKING_ATTENDERS, dtype=jnp.int32)
    ranking = jax.random.permutation(jax.random.fold_in(key, 41), ASKING_ATTENDERS)
    fast_count = ASKING_ATTENDERS // 2
    is_fast = ranking < fast_count
    fast_rate = jnp.exp(jax.random.uniform(jax.random.fold_in(key, 42), (ASKING_ATTENDERS,), jnp.float32, math.log(0.01), math.log(1.0 / 30.0)))
    slow_rate = jnp.exp(jax.random.uniform(jax.random.fold_in(key, 43), (ASKING_ATTENDERS,), jnp.float32, math.log(0.3), 0.0)) / CONTEXT_SPAN
    rate = jnp.where(is_fast, fast_rate, slow_rate)[:, None]
    block_factor = jnp.exp(jax.random.uniform(jax.random.fold_in(key, 44), (ASKING_ATTENDERS, N_EP), jnp.float32, math.log(0.5), math.log(2.0)))
    block_factor = jnp.repeat(block_factor, TOK_EP, axis=1)
    roughness = jax.random.uniform(jax.random.fold_in(key, 45), (ASKING_ATTENDERS, CONTEXT_SPAN), jnp.float32, 0.3, 1.7)
    doubling_rounds = -rate * block_factor * roughness
    span_offset = jax.random.randint(jax.random.fold_in(key, 46), (ASKING_ATTENDERS, 3), 0, CONTEXT_SPAN)
    span_extent = jax.random.uniform(jax.random.fold_in(key, 47), (ASKING_ATTENDERS, 3), jnp.float32, 0.22, 0.5)
    doubling_rounds = doubling_rounds.at[attender_ordinal[:, None], span_offset].add(-span_extent)
    return jnp.cumsum(doubling_rounds, axis=1)


def steps_of(key, dims, shards, low, top_value):
    factor_of, own = 1.0, jax.random.fold_in(key, 6)
    for position, shards_of in shards:
        heights = jnp.exp(jax.random.uniform(jax.random.fold_in(own, position), (shards_of,), jnp.float32, low / len(shards), top_value / len(shards)))
        factor_of = factor_of * jnp.repeat(heights, dims[position] // shards_of).reshape([-1 if axis == position else 1 for axis in range(len(dims))])
    return factor_of


def assign_block(stream_key, own, number, rows, amount, top, most, slope):
    order = jax.random.permutation(stream_key, amount)
    crowded, ordinary = shares(amount, rows * top, most, slope, True), shares(amount, rows * top, most, slope, False)
    places = jnp.arange(amount)

    def named(sizes, turn):
        used = int((sizes > 0).sum())
        fixed = max(1, used // 4)
        shifted = fixed + (places - fixed + turn * (used - fixed)) % max(1, amount - fixed)
        return jnp.zeros((amount,), jnp.int32).at[order[jnp.where(places < fixed, places, shifted)]].set(jnp.asarray(sizes, jnp.int32))

    sizes = jnp.where(number % 4 == 0, named(crowded, number // 4), named(ordinary, number - number // 4 - 1))
    mixed = jax.random.permutation(jax.random.fold_in(own, 3), amount)
    source_of, sink = mixed[0:amount // 2 * 2:2], mixed[1:amount // 2 * 2:2]
    margin = jnp.minimum(sizes[source_of] - 1, most - sizes[sink]) // 2
    margin = jnp.where((source_of == order[0]) | (sink == order[0]) | (sizes[sink] == 0), 0, jnp.maximum(margin, 0))
    shifted = jax.random.randint(jax.random.fold_in(own, 4), (amount // 2,), 0, 1 << 20) % (margin + 1)
    sizes = sizes.at[source_of].add(-shifted).at[sink].add(shifted)
    items = jnp.searchsorted(jnp.cumsum(sizes), jnp.arange(rows * top), side="right").astype(jnp.int32)
    grid = items.reshape(top, rows).T
    grid = grid[jax.random.permutation(jax.random.fold_in(own, 1), rows)]
    turn = jax.random.randint(jax.random.fold_in(own, 2), (rows, 1), 0, top)
    return jnp.take_along_axis(grid, (jnp.arange(top)[None, :] + turn) % top, axis=1)


def shares(number_of, total, limit, slope, full):
    weights = [(1 << 20) // math.isqrt(grade ** slope) + 1 for grade in range(1, number_of + 1)]
    largest = limit if full else min(limit, max(-(-total // number_of), total * weights[0] // sum(weights)))
    least = 1 if total - largest >= number_of - 1 else 0
    given, spare = [largest] + [least] * (number_of - 1), total - largest - least * (number_of - 1)
    while spare > 0:
        movable = [i for i in range(1, number_of) if given[i] < largest] or [i for i in range(1, number_of) if given[i] < limit]
        pool, budget = sum([weights[i] for i in movable]), spare
        for i in movable:
            extra = min(limit - given[i], max(1, budget * weights[i] // pool), spare)
            given[i] = given[i] + extra
            spare = spare - extra
    return np.array(given)


def gaussian(rng, shape, deviation, limit, pieces=(), kind=jnp.bfloat16):
    values = deviation * jax.random.normal(rng, shape, jnp.float32)
    if pieces:
        values = values * steps_of(rng, shape, pieces, -0.22, 0.18)
    return jnp.clip(values, -limit, limit).astype(kind)


def setup_inputs(seed: int = 0) -> dict:
    seeds = jax.random.split(jax.random.key(seed), 13)
    queries = draw_queries(jax.random.fold_in(seeds[12], 71), 0)
    keys_values = draw_keys_values(jax.random.fold_in(seeds[12], 71), 0)
    log_gate_cum = draw_log_gate_cum(jax.random.fold_in(seeds[12], 71), 0)
    mix_weight = gaussian(seeds[3], (ASKING_ATTENDERS * HEAD, D), (ASKING_ATTENDERS * HEAD) ** -0.5, 0.1875, ((0, 4),))
    mix_gain = jnp.clip(1.0 + 0.18 * jax.random.normal(seeds[4], (D,), jnp.float32), 0.1, 1.9)
    moe_in = gaussian(seeds[5], (TOKENS_M, D), 1.0, 6.0, ((0, 256),))
    moe_gain = jnp.clip(1.0 + 0.18 * jax.random.normal(seeds[6], (D,), jnp.float32), 0.1, 1.9)
    routes_keys = jax.random.split(jax.random.fold_in(seeds[7], 1), TOKENS_M // TOK_M)
    routes_turns = jax.random.permutation(jax.random.fold_in(seeds[7], 3), TOKENS_M // TOK_M)
    routes = jax.vmap(lambda own, number: assign_block(jax.random.fold_in(seeds[7], 2), own, number, TOK_M, EXPERTS, TOPK, CAP, 2))(routes_keys, routes_turns).reshape((TOKENS_M, TOPK))
    route_weight = jnp.clip(jnp.exp(math.log(2.0) - 2.0794415 * jax.random.uniform(seeds[8], (TOKENS_M, TOPK), jnp.float32) ** steps_of(seeds[8], (TOKENS_M, TOPK), ((0, 256),), -0.2, 0.2)), 0.25, 2.0)
    expert_gate = gaussian(seeds[9], (EXPERTS, D, FF), D ** -0.5, 0.125, ((0, 64), (2, 4)))
    expert_up = gaussian(seeds[10], (EXPERTS, D, FF), D ** -0.5, 0.125, ((0, 64), (2, 4)))
    expert_down = gaussian(seeds[11], (EXPERTS, FF, D), FF ** -0.5, 0.1875, ((0, 64), (1, 4)))
    return dict(queries=queries, keys_values=keys_values, log_gate_cum=log_gate_cum, mix_weight=mix_weight, mix_gain=mix_gain, moe_in=moe_in, moe_gain=moe_gain, routes=routes, route_weight=route_weight, expert_gate=expert_gate, expert_up=expert_up, expert_down=expert_down)


EPSILON = 1e-06

def rms_scale(values, gain):
    widened = values.astype(jnp.float32)
    return widened * lax.rsqrt(lax.optimization_barrier(jnp.mean(widened * widened, axis=-1, keepdims=True)) + EPSILON) * gain

def attend_reference(queries, keys_values, log_gate_cum):
    seq_len = queries.shape[0]
    group_size = ASKING_ATTENDERS // KV_HEADS
    block_rows = math.gcd(seq_len, 256)
    paired = keys_values.reshape(seq_len, KV_HEADS, 2, HEAD).astype(jnp.float32)
    key_part = paired[:, :, 0]
    value_part = paired[:, :, 1]
    gates = log_gate_cum.reshape(KV_HEADS, group_size, seq_len)
    key_pos = jnp.arange(seq_len, dtype=jnp.int32)

    def one_block(block_index):
        first_row = block_index * block_rows
        query_block = lax.dynamic_slice_in_dim(queries, first_row, block_rows, 0)
        query_block = query_block.reshape(block_rows, KV_HEADS, group_size, HEAD).astype(jnp.float32)
        scores = jnp.einsum('tgrd,ngd->grtn', query_block, key_part) * HEAD ** (-0.5)
        query_gate = lax.dynamic_slice_in_dim(gates, first_row, block_rows, 2)
        scores = scores + query_gate[..., None] - gates[:, :, None, :]
        query_pos = first_row + jnp.arange(block_rows, dtype=jnp.int32)
        causal = key_pos[None, :] <= query_pos[:, None]
        scores = jnp.where(causal, scores, -jnp.inf)
        row_max = lax.optimization_barrier(jnp.max(scores, axis=-1, keepdims=True))
        weight = jnp.exp(scores - row_max)
        row_total = lax.optimization_barrier(jnp.sum(weight, axis=-1))
        weight_b = lax.optimization_barrier(weight.astype(jnp.bfloat16)).astype(jnp.float32)
        mixed_heads = jnp.einsum('grtn,ngd->grtd', weight_b, value_part) / row_total[..., None]
        mixed_heads = jnp.transpose(mixed_heads, (2, 0, 1, 3)).reshape(block_rows, ASKING_ATTENDERS * HEAD)
        return mixed_heads.astype(jnp.bfloat16)
    blocks = lax.map(one_block, jnp.arange(seq_len // block_rows, dtype=jnp.int32))
    return blocks.reshape(seq_len, ASKING_ATTENDERS * HEAD)

def reference(queries, keys_values, log_gate_cum, mix_weight, mix_gain, moe_in, moe_gain, routes, route_weight, expert_gate, expert_up, expert_down):
    attended = attend_reference(queries, keys_values, log_gate_cum)
    seq_len = attended.shape[0]
    head_width = ASKING_ATTENDERS * HEAD // N_TP
    projected = jnp.zeros((seq_len, D), jnp.float32)
    for shard_index in range(N_TP):
        head_part = jnp.dot(attended[:, shard_index * head_width:(shard_index + 1) * head_width], mix_weight[shard_index * head_width:(shard_index + 1) * head_width], preferred_element_type=jnp.float32).astype(jnp.bfloat16)
        projected = projected + lax.optimization_barrier(head_part).astype(jnp.float32)
    mix_result = rms_scale(projected, mix_gain).astype(jnp.bfloat16)
    normed = rms_scale(moe_in, moe_gain).astype(jnp.bfloat16)
    token_count = normed.shape[0]
    flat_routes = routes.reshape(-1).astype(jnp.int32)
    flat_weight = route_weight.reshape(-1)
    order = jnp.argsort(flat_routes, stable=True).astype(jnp.int32)
    most_rows = N_EP * N_TP * CAP
    expert_ids = jnp.arange(EXPERTS, dtype=jnp.int32)
    counts = lax.optimization_barrier(jnp.sum((flat_routes[:, None] == expert_ids[None, :]).astype(jnp.int32), axis=0))
    starts = (jnp.cumsum(counts) - counts).astype(jnp.int32)
    order_padded = jnp.concatenate([order, jnp.zeros((most_rows,), jnp.int32)])
    ff_width = FF // N_TP

    def one_expert(accum, inputs):
        gate_here, up_here, down_here, first_slot, count_here = inputs
        picked = lax.dynamic_slice_in_dim(order_padded, first_slot, most_rows, 0)
        valid = jnp.arange(most_rows, dtype=jnp.int32) < count_here
        token_ids = (picked // TOPK).astype(jnp.int32)
        rows_in = normed[token_ids]
        hidden = (jax.nn.silu(jnp.dot(rows_in, gate_here, preferred_element_type=jnp.float32)) * jnp.dot(rows_in, up_here, preferred_element_type=jnp.float32)).astype(jnp.bfloat16)
        summed = jnp.zeros((most_rows, D), jnp.float32)
        for shard_index in range(N_TP):
            width_part = jnp.dot(hidden[:, shard_index * ff_width:(shard_index + 1) * ff_width], down_here[shard_index * ff_width:(shard_index + 1) * ff_width], preferred_element_type=jnp.float32).astype(jnp.bfloat16)
            summed = summed + lax.optimization_barrier(width_part).astype(jnp.float32)
        expert_out = lax.optimization_barrier(summed.astype(jnp.bfloat16)).astype(jnp.float32)
        scaled = jnp.where(valid, flat_weight[picked], 0.0)
        accum = accum.at[token_ids].add(scaled[:, None] * expert_out)
        return (accum, None)
    accum, _ = lax.scan(one_expert, jnp.zeros((token_count, D), jnp.float32), (expert_gate, expert_up, expert_down, starts, counts))
    moe_result = accum.astype(jnp.bfloat16)
    return (mix_result, moe_result)
```

```python
import functools

import jax
import jax.numpy as jnp
from jax import lax
from jax.experimental import pallas as pl
from jax.experimental.pallas import tpu as pltpu
from jax.sharding import PartitionSpec as P

HEAD = 64
EPSILON = 1e-06
NEGATIVE = -3e38
LANES = 128
KEY_BLOCK = 512
MESH = pl.DeviceIdType.MESH
F32 = jnp.float32
BF16 = jnp.bfloat16


def dot(a, b):
    return jnp.dot(a, b, preferred_element_type=F32)


def rms_scale(values, gain):
    return values * lax.rsqrt(jnp.mean(values * values, axis=-1, keepdims=True) + EPSILON) * gain


def pack_kernel(capacity, x_ref, gain_ref, routes_ref, out_ref, wide):
    rows, width = x_ref.shape
    tiles = width // LANES
    slots = out_ref.shape[0] // tiles
    experts = slots // capacity
    normed = rms_scale(x_ref[...].astype(F32), gain_ref[...]).astype(BF16)
    ids = lax.broadcasted_iota(jnp.int32, (experts, rows), 0)
    first = (ids == routes_ref[0:1, :]).astype(F32)
    second = (ids == routes_ref[1:2, :]).astype(F32)
    upper = (
        lax.broadcasted_iota(jnp.int32, (rows, rows), 0)
        < lax.broadcasted_iota(jnp.int32, (rows, rows), 1)
    ).astype(BF16)
    first_before = dot(first.astype(BF16), upper)
    second_before = dot(second.astype(BF16), upper) + jnp.sum(first, axis=1, keepdims=True)
    first_pos = jnp.sum(first * first_before, axis=0, keepdims=True).astype(jnp.int32)
    second_pos = jnp.sum(second * second_before, axis=0, keepdims=True).astype(jnp.int32)
    slot_ids = lax.broadcasted_iota(jnp.int32, (slots, rows), 0)
    pick = jnp.where(
        (slot_ids == routes_ref[0:1, :] * capacity + first_pos)
        | (slot_ids == routes_ref[1:2, :] * capacity + second_pos),
        1.0,
        0.0,
    ).astype(BF16)
    for half in range(tiles // 2):
        moved = dot(pick, normed[:, half * 2 * LANES : (half + 1) * 2 * LANES])
        wide[pl.ds(2 * half, slots, stride=tiles), :] = moved[:, :LANES]
        wide[pl.ds(2 * half + 1, slots, stride=tiles), :] = moved[:, LANES:]
    out_ref[...] = wide[...].astype(BF16)


def unpack_kernel(
    capacity, ret_ref, routes_ref, weight_ref, mix_ref, gain_ref, mix_out, moe_out, wide
):
    rows, width = moe_out.shape
    tiles = width // LANES
    slots = ret_ref.shape[0] // tiles
    experts = slots // capacity
    wide[...] = ret_ref[...].astype(F32)
    ids = lax.broadcasted_iota(jnp.int32, (rows, experts), 1)
    first = (ids == routes_ref[:, 0:1]).astype(F32)
    second = (ids == routes_ref[:, 1:2]).astype(F32)
    lower = (
        lax.broadcasted_iota(jnp.int32, (rows, rows), 1)
        < lax.broadcasted_iota(jnp.int32, (rows, rows), 0)
    ).astype(BF16)
    first_before = dot(lower, first.astype(BF16))
    second_before = dot(lower, second.astype(BF16)) + jnp.sum(first, axis=0, keepdims=True)
    first_pos = jnp.sum(first * first_before, axis=1, keepdims=True).astype(jnp.int32)
    second_pos = jnp.sum(second * second_before, axis=1, keepdims=True).astype(jnp.int32)
    slot_ids = lax.broadcasted_iota(jnp.int32, (rows, slots), 1)
    first_pick = jnp.where(
        slot_ids == routes_ref[:, 0:1] * capacity + first_pos, 1.0, 0.0
    ).astype(BF16)
    second_pick = jnp.where(
        slot_ids == routes_ref[:, 1:2] * capacity + second_pos, 1.0, 0.0
    ).astype(BF16)
    for half in range(tiles // 2):
        block = jnp.concatenate(
            [wide[pl.ds(2 * half + side, slots, stride=tiles), :] for side in (0, 1)], axis=1
        ).astype(BF16)
        total = weight_ref[:, 0:1] * dot(first_pick, block)
        total = total + weight_ref[:, 1:2] * dot(second_pick, block)
        moe_out[:, half * 2 * LANES : (half + 1) * 2 * LANES] = total.astype(BF16)
    summed = mix_ref[0].astype(F32)
    for part in range(1, mix_ref.shape[0]):
        summed = summed + mix_ref[part].astype(F32)
    mix_out[...] = rms_scale(summed, gain_ref[...]).astype(BF16)


def main_kernel(
    planes,
    columns,
    send_ref,
    q_ref,
    kv_ref,
    gate_log_ref,
    mixw_ref,
    gate_ref,
    up_ref,
    down_ref,
    ret_ref,
    mixr_ref,
    wg,
    wu,
    wd,
    kvb,
    recv,
    xs,
    hid,
    wide,
    outb,
    qs,
    m_ref,
    l_ref,
    acc_ref,
    mixb,
    own_sem,
    wsend,
    wrecv,
    kzsend,
    kzrecv,
    kxsend,
    kxrecv,
    kcsend,
    kcrecv,
    dsend,
    drecv,
    csend,
    crecv,
    msend,
    mrecv,
):
    ep = planes * columns * 2
    tp = 4
    me = lax.axis_index("ep")
    my = lax.axis_index("tp")
    my_z = me // (2 * columns)
    my_x = (me // 2) % columns
    my_c = me % 2
    right, left = (my + 1) % tp, (my + 3) % tp
    far = (my + 2) % tp
    chunk = send_ref.shape[0] // ep
    queries = q_ref.shape[0]
    heads = q_ref.shape[1] // HEAD
    model = down_ref.shape[1]
    tiles = model // LANES

    def at(e, t=None):
        return {"ep": e, "tp": my if t is None else t}

    barrier = pltpu.get_barrier_semaphore()

    def greet_ep(k, carry):
        pl.semaphore_signal(barrier, inc=1, device_id=at((me + k) % ep), device_id_type=MESH)
        return carry

    lax.fori_loop(1, ep, greet_ep, 0)
    for k in range(1, tp):
        pl.semaphore_signal(barrier, inc=1, device_id=at(me, (my + k) % tp), device_id_type=MESH)
    pl.semaphore_wait(barrier, ep - 1 + tp - 1)

    def remote(src, dst, s_sem, r_sem, where):
        return pltpu.make_async_remote_copy(
            src_ref=src, dst_ref=dst, send_sem=s_sem, recv_sem=r_sem, device_id=where,
            device_id_type=MESH,
        )

    mats = ((gate_ref, wg), (up_ref, wu), (down_ref, wd))
    near = {}
    for m, (src, dst) in enumerate(mats):
        for way, peer in enumerate((right, left)):
            near[m, way] = remote(
                src, dst.at[my], wsend.at[way, m, 0], wrecv.at[way, m, 0], at(me, peer)
            )
            near[m, way].start()

    def kv_slot(z, x, c):
        return (z * columns + x) * 2 + c

    def z_copy(k):
        z = (my_z + k) % planes
        return remote(
            kv_ref, kvb.at[me], kzsend.at[k], kzrecv.at[k], at(kv_slot(z, my_x, my_c))
        )

    for k in range(1, planes):
        z_copy(k).start()

    def dispatch(k):
        e = (me + k) % ep
        return remote(
            send_ref.at[pl.ds(pl.multiple_of(e * chunk, 16), chunk)],
            recv.at[pl.ds(pl.multiple_of(me * chunk, 16), chunk)],
            dsend.at[k],
            drecv.at[k],
            at(e),
        )

    def start_dispatch(k, carry):
        dispatch(k).start()
        return carry

    lax.fori_loop(1, ep, start_dispatch, 0)

    own = [
        pltpu.make_async_copy(src, dst.at[my], own_sem.at[m]) for m, (src, dst) in enumerate(mats)
    ]
    for copy in own:
        copy.start()
    kvb[me] = kv_ref[...]
    mine = pl.ds(pl.multiple_of(me * chunk, 16), chunk)
    recv[mine, :] = send_ref[mine, :]

    for h in range(heads):
        part = q_ref[:, h * HEAD : (h + 1) * HEAD].astype(F32) * HEAD ** (-0.5)
        qs[h] = jnp.concatenate([part, jnp.zeros_like(part)], axis=1).astype(BF16)
        m_ref[h] = jnp.full((queries, LANES), NEGATIVE, F32)
        l_ref[h] = jnp.zeros((queries, LANES), F32)
        acc_ref[h] = jnp.zeros((queries, LANES), F32)

    def x_copy(k, j):
        slab = kvb.at[kv_slot((my_z + planes - j) % planes, my_x, my_c)]
        return remote(
            slab,
            slab,
            kxsend.at[k * planes + j],
            kxrecv.at[k * planes + j],
            at(kv_slot(my_z, (my_x + k) % columns, my_c)),
        )

    def c_copy(k, j):
        slab = kvb.at[kv_slot((my_z + planes - j) % planes, (my_x + columns - k) % columns, my_c)]
        return remote(
            slab, slab, kcsend.at[k * planes + j], kcrecv.at[k * planes + j], at(me + 1 - 2 * my_c)
        )

    for j in range(planes):
        if j > 0:
            z_copy(j).wait_recv()
        for k in range(1, columns):
            x_copy(k, j).start()
        c_copy(0, j).start()

    def pass_on(j, carry):
        for k in range(1, columns):
            x_copy(k, j).wait_recv()
            c_copy(k, j).start()
        return carry

    lax.fori_loop(0, planes, pass_on, 0)

    def far_copy(m, way):
        dst = mats[m][1]
        source = left if way == 0 else right
        peer = right if way == 0 else left
        half = dst.shape[1] // 2
        block = dst.at[source, pl.ds(way * half, half)]
        return remote(block, block, wsend.at[way, m, 1], wrecv.at[way, m, 1], at(me, peer))

    for m in (0, 1):
        for way in (0, 1):
            near[m, way].wait_recv()
            far_copy(m, way).start()

    def wait_c(j, carry):
        c_copy(0, j).wait_recv()
        for k in range(1, columns):
            c_copy(k, j).wait_recv()
        return carry

    lax.fori_loop(0, planes, wait_c, 0)

    base = gate_log_ref[:, pl.ds(pl.multiple_of(me * queries, LANES), LANES)][:, 0:1]
    slabs = KEY_BLOCK // queries

    def attend(i, masked):
        keys = kvb[pl.ds(i * slabs, slabs)].reshape(KEY_BLOCK, 2 * HEAD)
        start = pl.multiple_of(i * KEY_BLOCK, KEY_BLOCK)
        bias = base - gate_log_ref[:, pl.ds(start, KEY_BLOCK)]
        for h in range(heads):
            scores = lax.dot_general(
                qs[h], keys, (((1,), (1,)), ((), ())), preferred_element_type=F32
            )
            scores = scores + bias[h : h + 1, :]
            if masked:
                key_pos = start + lax.broadcasted_iota(jnp.int32, scores.shape, 1)
                query_pos = me * queries + lax.broadcasted_iota(jnp.int32, scores.shape, 0)
                scores = jnp.where(key_pos <= query_pos, scores, NEGATIVE)
            old = m_ref[h]
            new = jnp.maximum(old, jnp.max(scores, axis=1, keepdims=True))
            factor = jnp.exp(old - new)
            weight = jnp.exp(scores - jnp.concatenate([new] * (KEY_BLOCK // LANES), axis=1))
            part = weight[:, :LANES]
            for t in range(1, KEY_BLOCK // LANES):
                part = part + weight[:, t * LANES : (t + 1) * LANES]
            m_ref[h] = new
            l_ref[h] = l_ref[h] * factor + part
            acc_ref[h] = acc_ref[h] * factor + dot(weight.astype(BF16), keys)

    full = me // slabs

    def attend_full(i, carry):
        attend(i, False)
        return carry

    lax.fori_loop(0, full, attend_full, 0)
    attend(full, True)

    for way in (0, 1):
        near[2, way].wait_recv()
        far_copy(2, way).start()

    attended = jnp.concatenate(
        [acc_ref[h][:, HEAD:] / jnp.sum(l_ref[h], axis=1, keepdims=True) for h in range(heads)],
        axis=1,
    ).astype(BF16)
    mixb[...] = dot(attended, mixw_ref[...]).astype(BF16)
    share = queries // tp

    def mix_copy(k):
        t = (my + k) % tp
        return remote(
            mixb.at[pl.ds(pl.multiple_of(t * share, 16), share)],
            mixr_ref.at[k],
            msend.at[k],
            mrecv.at[k],
            at(me, t),
        )

    for k in range(1, tp):
        mix_copy(k).start()
    mixr_ref[0] = mixb[pl.ds(pl.multiple_of(my * share, 16), share), :]

    def wait_dispatch(k, carry):
        dispatch(k).wait_recv()
        return carry

    lax.fori_loop(1, ep, wait_dispatch, 0)
    groups = 4
    group_rows = xs.shape[0] // groups
    group_tiles = group_rows * tiles

    def spread(g, carry):
        wide[...] = recv[pl.ds(pl.multiple_of(g * group_tiles, 16), group_tiles), :].astype(F32)
        rows = pl.ds(pl.multiple_of(g * group_rows, 16), group_rows)
        for j in range(tiles):
            xs[rows, j * LANES : (j + 1) * LANES] = wide[
                pl.ds(j, group_rows, stride=tiles), :
            ].astype(BF16)
        return carry

    lax.fori_loop(0, groups, spread, 0)

    for copy in own:
        copy.wait()

    def expand(q):
        up_part = dot(xs[...], wu[q])
        gate_part = dot(xs[...], wg[q])
        hid[q] = (gate_part / (1.0 + jnp.exp(-gate_part)) * up_part).astype(BF16)

    for m in (0, 1):
        for way in (0, 1):
            far_copy(m, way).wait_recv()

    def expand_step(q, carry):
        expand(q)
        return carry

    lax.fori_loop(0, tp, expand_step, 0)
    for way in (0, 1):
        far_copy(2, way).wait_recv()

    per_group = ep // groups
    cols = 4 * LANES

    def combine(s, k):
        return remote(
            outb.at[pl.ds(pl.multiple_of(s * chunk, 16), chunk)],
            ret_ref.at[pl.ds(pl.multiple_of(me * chunk, 16), chunk)],
            csend.at[k],
            crecv.at[k],
            at(s),
        )

    def contract(i, carry):
        g = (i + me // per_group) % groups
        rows = pl.ds(pl.multiple_of(g * group_rows, 16), group_rows)
        for n in range(model // cols):
            total = jnp.zeros((group_rows, cols), F32)
            for q in range(tp):
                total = total + dot(hid[q, rows, :], wd[q, :, n * cols : (n + 1) * cols])
            for j in range(4):
                wide[pl.ds(n * 4 + j, group_rows, stride=tiles), :] = total[
                    :, j * LANES : (j + 1) * LANES
                ]
        outb[pl.ds(pl.multiple_of(g * group_tiles, 16), group_tiles), :] = wide[...].astype(BF16)

        def start_combine(j, carry):
            s = g * per_group + (j + me) % per_group

            @pl.when(s != me)
            def _():
                combine(s, (s + ep - me) % ep).start()

            return carry

        lax.fori_loop(0, per_group, start_combine, 0)
        return carry

    lax.fori_loop(0, groups, contract, 0)
    ret_ref[mine, :] = outb[mine, :]

    for k in range(1, tp):
        mix_copy(k).wait()

    def wait_combine(k, carry):
        combine((me + k) % ep, k).wait()
        dispatch(k).wait_send()
        return carry

    lax.fori_loop(1, ep, wait_combine, 0)
    for k in range(1, planes):
        z_copy(k).wait_send()

    def wait_kv(j, carry):
        c_copy(0, j).wait_send()
        for k in range(1, columns):
            x_copy(k, j).wait_send()
            c_copy(k, j).wait_send()
        return carry

    lax.fori_loop(0, planes, wait_kv, 0)
    for m in range(3):
        for way in (0, 1):
            near[m, way].wait_send()
            far_copy(m, way).wait_send()


def body(
    planes,
    columns,
    queries,
    keys_values,
    log_gate_cum,
    mix_weight,
    mix_gain,
    moe_in,
    moe_gain,
    routes,
    route_weight,
    expert_gate,
    expert_up,
    expert_down,
):
    ep = planes * columns * 2
    tp = 4
    tokens, model = moe_in.shape
    tiles = model // LANES
    capacity = 3 * routes.shape[1] * tokens // (2 * ep)
    slots = ep * capacity
    rows = queries.shape[0]
    heads = queries.shape[1] // HEAD
    depth, width = expert_gate.shape[1:]
    vmem = pl.BlockSpec(memory_space=pltpu.VMEM)
    hbm = pl.BlockSpec(memory_space=pl.ANY)
    big = 64000 * 1024

    packed = pl.pallas_call(
        functools.partial(pack_kernel, capacity),
        out_shape=jax.ShapeDtypeStruct((slots * tiles, LANES), BF16),
        in_specs=[vmem] * 3,
        out_specs=vmem,
        scratch_shapes=[pltpu.VMEM((slots * tiles, LANES), F32)],
        compiler_params=pltpu.CompilerParams(vmem_limit_bytes=big // 2),
        name="pack",
    )(moe_in, moe_gain[None], routes.T)

    dma = pltpu.SemaphoreType.DMA
    returned, mixed = pl.pallas_call(
        functools.partial(main_kernel, planes, columns),
        out_shape=(
            jax.ShapeDtypeStruct((slots * tiles, LANES), BF16),
            jax.ShapeDtypeStruct((tp, rows // tp, model), BF16),
        ),
        in_specs=[vmem] * 5 + [hbm] * 3,
        out_specs=(vmem, vmem),
        scratch_shapes=[
            pltpu.VMEM((tp, depth, width), BF16),
            pltpu.VMEM((tp, depth, width), BF16),
            pltpu.VMEM((tp, width, model), BF16),
            pltpu.VMEM((ep, rows, 2 * HEAD), BF16),
            pltpu.VMEM((slots * tiles, LANES), BF16),
            pltpu.VMEM((slots, model), BF16),
            pltpu.VMEM((tp, slots, width), BF16),
            pltpu.VMEM((slots * tiles // 4, LANES), F32),
            pltpu.VMEM((slots * tiles, LANES), BF16),
            pltpu.VMEM((heads, rows, 2 * HEAD), BF16),
            pltpu.VMEM((heads, rows, LANES), F32),
            pltpu.VMEM((heads, rows, LANES), F32),
            pltpu.VMEM((heads, rows, LANES), F32),
            pltpu.VMEM((rows, model), BF16),
            dma((3,)),
            dma((2, 3, 2)),
            dma((2, 3, 2)),
            dma((planes,)),
            dma((planes,)),
            dma((columns * planes,)),
            dma((columns * planes,)),
            dma((columns * planes,)),
            dma((columns * planes,)),
            dma((ep,)),
            dma((ep,)),
            dma((ep,)),
            dma((ep,)),
            dma((tp,)),
            dma((tp,)),
        ],
        compiler_params=pltpu.CompilerParams(
            collective_id=0, has_side_effects=True, vmem_limit_bytes=big
        ),
        name="exchange",
    )(
        packed,
        queries,
        keys_values,
        log_gate_cum,
        mix_weight,
        expert_gate[0],
        expert_up[0],
        expert_down[0],
    )

    return pl.pallas_call(
        functools.partial(unpack_kernel, capacity),
        out_shape=(
            jax.ShapeDtypeStruct((rows // tp, model), BF16),
            jax.ShapeDtypeStruct((tokens, model), BF16),
        ),
        in_specs=[vmem] * 5,
        out_specs=(vmem, vmem),
        scratch_shapes=[pltpu.VMEM((slots * tiles, LANES), F32)],
        compiler_params=pltpu.CompilerParams(vmem_limit_bytes=big // 2),
        name="unpack",
    )(returned, routes, route_weight, mixed, mix_gain[None])


def solution(mesh, planes=8, columns=4):
    in_specs = (
        P("ep", "tp"),
        P("ep", "tp"),
        P("tp", None),
        P("tp", None),
        P(),
        P(("ep", "tp"), None),
        P(),
        P(("ep", "tp"), None),
        P(("ep", "tp"), None),
        P("ep", None, "tp"),
        P("ep", None, "tp"),
        P("ep", "tp", None),
    )
    out_specs = (P(("ep", "tp"), None), P(("ep", "tp"), None))
    return jax.shard_map(
        functools.partial(body, planes, columns),
        mesh=mesh,
        in_specs=in_specs,
        out_specs=out_specs,
        check_vma=False,
    )
```

```python
import functools

import jax
import jax.numpy as jnp
from jax import lax
from jax.experimental import pallas as pl
from jax.experimental.pallas import tpu as pltpu
from jax.sharding import PartitionSpec as P

HEAD = 64
EPSILON = 1e-06
NEGATIVE = -3e38
LANES = 128
KEY_BLOCK = 512
GROUPS = 4
PIECES = (0, 32, 64, 96, 144)
MESH = pl.DeviceIdType.MESH
F32 = jnp.float32
BF16 = jnp.bfloat16


def dot(a, b):
    return jnp.dot(a, b, preferred_element_type=F32)


def rms_scale(values, gain):
    return values * lax.rsqrt(jnp.mean(values * values, axis=-1, keepdims=True) + EPSILON) * gain


def step_kernel(
    planes,
    columns,
    q_hbm,
    kv_hbm,
    gate_log_hbm,
    mixw_hbm,
    mix_gain_ref,
    x_hbm,
    moe_gain_ref,
    routes_ref,
    weight_ref,
    gate_hbm,
    up_hbm,
    down_hbm,
    mix_out,
    moe_out,
    x_ref,
    q_ref,
    gate_log_ref,
    mixw_ref,
    wg,
    wu,
    wd,
    kvb,
    picks,
    send,
    recv,
    xs,
    hid,
    wide,
    outb,
    ret,
    qs,
    m_ref,
    l_ref,
    acc_ref,
    mixb,
    mixr,
    own_sem,
    wsend,
    wrecv,
    kzsend,
    kzrecv,
    kxsend,
    kxrecv,
    kcsend,
    kcrecv,
    dsend,
    drecv,
    csend,
    crecv,
    msend,
    mrecv,
):
    ep = planes * columns * 2
    tp = 4
    me = lax.axis_index("ep")
    my = lax.axis_index("tp")
    my_z = me // (2 * columns)
    my_x = (me // 2) % columns
    my_c = me % 2
    tokens, model = x_ref.shape
    tiles = model // LANES
    slots = xs.shape[0]
    capacity = slots // ep
    chunk = capacity * tiles
    per_group = ep // GROUPS
    group_rows = slots // GROUPS
    my_group = me // per_group
    queries = q_ref.shape[0]
    heads = q_ref.shape[1] // HEAD

    def at(e, t=None):
        return {"ep": e, "tp": my if t is None else t}

    def remote(src, dst, s_sem, r_sem, where):
        return pltpu.make_async_remote_copy(
            src_ref=src,
            dst_ref=dst,
            send_sem=s_sem,
            recv_sem=r_sem,
            device_id=where,
            device_id_type=MESH,
        )

    barrier = pltpu.get_barrier_semaphore()

    def greet_ep(k, carry):
        pl.semaphore_signal(barrier, inc=1, device_id=at((me + k) % ep), device_id_type=MESH)
        return carry

    lax.fori_loop(1, ep, greet_ep, 0)
    for k in range(1, tp):
        pl.semaphore_signal(barrier, inc=1, device_id=at(me, (my + k) % tp), device_id_type=MESH)

    own = [
        pltpu.make_async_copy(src, dst, own_sem.at[i])
        for i, (src, dst) in enumerate(
            (
                (x_hbm, x_ref),
                (kv_hbm, kvb.at[me]),
                (q_hbm, q_ref),
                (gate_log_hbm, gate_log_ref),
                (mixw_hbm, mixw_ref),
                (gate_hbm, wg.at[my]),
                (up_hbm, wu.at[my]),
                (down_hbm, wd.at[my]),
            )
        )
    ]
    for copy in own:
        copy.start()

    ids = lax.broadcasted_iota(jnp.int32, (tokens, ep), 1)
    lower = (
        lax.broadcasted_iota(jnp.int32, (tokens, tokens), 1)
        < lax.broadcasted_iota(jnp.int32, (tokens, tokens), 0)
    ).astype(BF16)
    slot_ids = lax.broadcasted_iota(jnp.int32, (tokens, slots), 1)
    taken = jnp.zeros((1, ep), F32)
    routes = routes_ref[...].T
    for side in range(2):
        expert = routes[:, side : side + 1]
        named = (ids == expert).astype(F32)
        before = dot(lower, named.astype(BF16)) + taken
        taken = taken + jnp.sum(named, axis=0, keepdims=True)
        position = jnp.sum(named * before, axis=1, keepdims=True).astype(jnp.int32)
        slot = (expert // per_group) * group_rows + position * per_group + expert % per_group
        picks[side] = jnp.where(slot_ids == slot, 1.0, 0.0).astype(BF16)

    pl.semaphore_wait(barrier, ep - 1 + tp - 1)

    ends = [-(-b // capacity) * LANES for b in PIECES]
    stages = [(gate_hbm, wg, None), (up_hbm, wu, None)] + [
        (down_hbm, wd, pl.ds(a, b - a)) for a, b in zip(ends[:-1], ends[1:])
    ]

    def part_of(i, source, half=None):
        src, dst, cols = stages[i]
        if half is None:
            return (src, dst.at[source]) if cols is None else (
                src.at[:, cols], dst.at[source, :, cols]
            )
        size = dst.shape[1] // 2
        band = pl.ds(half * size, size)
        block = dst.at[source, band] if cols is None else dst.at[source, band, cols]
        return block, block

    def near(i, way):
        src, dst = part_of(i, my)
        peer = (my + (1, 3)[way]) % tp
        return remote(src, dst, wsend.at[i, way], wrecv.at[i, way], at(me, peer))

    def far(i, way):
        src, dst = part_of(i, (my + (3, 1)[way]) % tp, way)
        peer = (my + (1, 3)[way]) % tp
        return remote(src, dst, wsend.at[i, 2 + way], wrecv.at[i, 2 + way], at(me, peer))

    def start_near(i):
        for way in (0, 1):
            near(i, way).start()

    def relay(i):
        for way in (0, 1):
            near(i, way).wait_recv()
            far(i, way).start()

    start_near(0)
    start_near(1)

    def kv_slot(z, x, c):
        return (z * columns + x) * 2 + c

    def z_copy(k):
        return remote(
            kv_hbm,
            kvb.at[me],
            kzsend.at[k],
            kzrecv.at[k],
            at(kv_slot((my_z + k) % planes, my_x, my_c)),
        )

    for k in range(1, planes):

        @pl.when(my_z + k < planes)
        def _(k=k):
            z_copy(k).start()

    own[0].wait()
    normed = rms_scale(x_ref[...].astype(F32), moe_gain_ref[...]).astype(BF16)
    both = picks[0] + picks[1]

    def lay_out(g, value, first):
        for j in range(value.shape[1] // LANES):
            for r in range(capacity):
                wide[g, pl.ds((first + j) * capacity + r, per_group, stride=chunk), :] = value[
                    r * per_group : (r + 1) * per_group, j * LANES : (j + 1) * LANES
                ]

    def gather_up(g, first, last):
        rows = pl.multiple_of(g * group_rows, 16)
        for j in range(first, last):
            for r in range(capacity):
                xs[pl.ds(rows + r * per_group, per_group), j * LANES : (j + 1) * LANES] = wide[
                    g, pl.ds(j * capacity + r, per_group, stride=chunk), :
                ].astype(BF16)

    for pair in range(tiles // 2):
        moved = lax.dot_general(
            both,
            normed[:, pair * 2 * LANES : (pair + 1) * 2 * LANES],
            (((0,), (0,)), ((), ())),
            preferred_element_type=F32,
        )
        for g in range(GROUPS):
            lay_out(g, moved[g * group_rows : (g + 1) * group_rows], 2 * pair)
    for g in range(GROUPS):
        send[g * per_group * chunk : (g + 1) * per_group * chunk, :] = wide[g].astype(BF16)

    def rows_of(e, start=0, size=chunk):
        return pl.ds(pl.multiple_of(e * chunk + start, 16), size)

    def start_dispatch(k, carry):
        e = (me + k) % ep
        remote(
            send.at[rows_of(e)], recv.at[rows_of(me)], dsend, drecv.at[my_group], at(e)
        ).start()
        return carry

    lax.fori_loop(1, ep, start_dispatch, 0)
    recv[rows_of(me), :] = send[rows_of(me), :]

    def amount(rows, sem):
        return pltpu.make_async_copy(send.at[pl.ds(0, rows)], recv.at[pl.ds(0, rows)], sem)

    for i in (1, 2, 3):
        own[i].wait()
    for h in range(heads):
        part = q_ref[:, h * HEAD : (h + 1) * HEAD].astype(F32) * HEAD ** (-0.5)
        qs[h * queries : (h + 1) * queries, :] = jnp.concatenate(
            [part, jnp.zeros_like(part)], axis=1
        ).astype(BF16)
        m_ref[h] = jnp.full((queries, LANES), NEGATIVE, F32)
        l_ref[h] = jnp.zeros((queries, LANES), F32)
        acc_ref[h] = jnp.zeros((queries, LANES), F32)

    def x_copy(k, j):
        slab = kvb.at[kv_slot((my_z + planes - j) % planes, my_x, my_c)]
        return remote(
            slab,
            slab,
            kxsend.at[k * planes + j],
            kxrecv.at[k * planes + j],
            at(kv_slot(my_z, (my_x + k) % columns, my_c)),
        )

    def c_copy(k, j):
        slab = kvb.at[kv_slot((my_z + planes - j) % planes, (my_x + columns - k) % columns, my_c)]
        return remote(
            slab, slab, kcsend.at[k * planes + j], kcrecv.at[k * planes + j], at(me + 1 - 2 * my_c)
        )

    base = gate_log_ref[:, pl.ds(pl.multiple_of(me * queries, LANES), LANES)][:, 0:1]
    slabs = KEY_BLOCK // queries

    def attend(i, masked):
        keys = kvb[pl.ds(i * slabs, slabs)].reshape(KEY_BLOCK, 2 * HEAD)
        start = pl.multiple_of(i * KEY_BLOCK, KEY_BLOCK)
        bias = base - gate_log_ref[:, pl.ds(start, KEY_BLOCK)]
        scores = lax.dot_general(
            qs[...], keys, (((1,), (1,)), ((), ())), preferred_element_type=F32
        )
        weights = []
        factors = []
        for h in range(heads):
            part = scores[h * queries : (h + 1) * queries] + bias[h : h + 1, :]
            if masked:
                key_pos = start + lax.broadcasted_iota(jnp.int32, part.shape, 1)
                query_pos = me * queries + lax.broadcasted_iota(jnp.int32, part.shape, 0)
                part = jnp.where(key_pos <= query_pos, part, NEGATIVE)
            old = m_ref[h]
            new = jnp.maximum(old, jnp.max(part, axis=1, keepdims=True))
            factor = jnp.exp(old - new)
            weight = jnp.exp(part - jnp.concatenate([new] * (KEY_BLOCK // LANES), axis=1))
            summed = weight[:, :LANES]
            for t in range(1, KEY_BLOCK // LANES):
                summed = summed + weight[:, t * LANES : (t + 1) * LANES]
            m_ref[h] = new
            l_ref[h] = l_ref[h] * factor + summed
            weights.append(weight.astype(BF16))
            factors.append(factor)
        moved = dot(jnp.concatenate(weights, axis=0), keys)
        for h in range(heads):
            acc_ref[h] = acc_ref[h] * factors[h] + moved[h * queries : (h + 1) * queries]

    def attend_step(t, carry):
        @pl.when(t <= my_z)
        def _():
            @pl.when(t > 0)
            def _():
                z_copy(t).wait_recv()

            for k in range(1, columns):
                x_copy(k, t).start()
            c_copy(0, t).start()

        @pl.when((t >= 1) & (t <= my_z + 1))
        def _():
            for k in range(1, columns):
                x_copy(k, t - 1).wait_recv()
                c_copy(k, t - 1).start()

        @pl.when(t == planes // 2 + 1)
        def _():
            relay(0)
            start_near(2)

        @pl.when(t >= 2)
        def _():
            for k in range(columns):
                c_copy(k, t - 2).wait_recv()
            first = (my_z + 2 - t) * columns

            def whole(i, carry):
                attend(i, False)
                return carry

            lax.fori_loop(first, first + jnp.where(t == 2, my_x, columns), whole, 0)

            @pl.when(t == 2)
            def _():
                attend(me // slabs, True)

        return carry

    lax.fori_loop(0, my_z + 3, attend_step, 0)

    @pl.when(my_z + 2 < planes // 2 + 1)
    def _():
        relay(0)
        start_near(2)

    relay(1)

    own[4].wait()
    attended = jnp.concatenate(
        [acc_ref[h][:, HEAD:] / jnp.sum(l_ref[h], axis=1, keepdims=True) for h in range(heads)],
        axis=1,
    ).astype(BF16)
    mixb[...] = dot(attended, mixw_ref[...]).astype(BF16)
    share = queries // tp

    def mix_copy(k):
        t = (my + k) % tp
        return remote(
            mixb.at[pl.ds(pl.multiple_of(t * share, 16), share)],
            mixr.at[k],
            msend.at[k],
            mrecv.at[k],
            at(me, t),
        )

    mixr[0] = mixb[pl.ds(pl.multiple_of(my * share, 16), share), :]

    for i in (5, 6, 7):
        own[i].wait()
    for g in range(GROUPS):

        @pl.when(g == my_group)
        def _(g=g):
            amount((per_group - 1) * chunk, drecv.at[g]).wait()

        @pl.when(g != my_group)
        def _(g=g):
            amount(per_group * chunk, drecv.at[g]).wait()

    def spread(g, carry):
        size = per_group * chunk
        wide[g] = recv[pl.ds(pl.multiple_of(g * size, 16), size), :].astype(F32)
        gather_up(g, 0, tiles)
        return carry

    lax.fori_loop(0, GROUPS, spread, 0)

    def expand(k, carry):
        q = (my + k) % tp
        up_part = dot(xs[...], wu[q])
        gate_part = dot(xs[...], wg[q])
        hid[q] = (gate_part / (1.0 + jnp.exp(-gate_part)) * up_part).astype(BF16)
        return carry

    def expand_step(i, carry):
        @pl.when(i == 3)
        def _():
            relay(2)
            for m in range(3, min(5, len(stages))):
                start_near(m)
            for m in (0, 1):
                for way in (0, 1):
                    far(m, way).wait_recv()

        return expand(i + (i // 2) * (5 - 2 * i), carry)

    lax.fori_loop(0, tp, expand_step, 0)

    pieces = list(zip(PIECES[:-1], PIECES[1:]))

    def contract(p, i):
        low, high = pieces[p]
        g = (i + my_group) % GROUPS
        rows = pl.ds(pl.multiple_of(g * group_rows, 16), group_rows)
        first, last = ends[p], ends[p + 1]
        total = jnp.zeros((group_rows, last - first), F32)
        for q in range(tp):
            total = total + dot(hid[q, rows, :], wd[q, :, first:last])
        lay_out(g, total, first // LANES)
        for s in range(per_group):
            outb[rows_of(g * per_group + s, low, high - low), :] = wide[
                g, s * chunk + low : s * chunk + high, :
            ].astype(BF16)

        def start_combine(j, carry):
            s = g * per_group + (j + me) % per_group

            @pl.when(s != me)
            def _():
                remote(
                    outb.at[rows_of(s, low, high - low)],
                    ret.at[rows_of(me, low, high - low)],
                    csend,
                    crecv.at[p],
                    at(s),
                ).start()

            return carry

        lax.fori_loop(0, per_group, start_combine, 0)

    for p in range(len(pieces)):
        if p > 0:
            relay(2 + p)
            if p + 2 < len(pieces):
                start_near(4 + p)
        if p == len(pieces) - 1:
            for k in range(1, tp):
                mix_copy(k).start()
        for way in (0, 1):
            far(2 + p, way).wait_recv()

        def contract_step(i, carry, p=p):
            contract(p, i)
            return carry

        lax.fori_loop(0, GROUPS, contract_step, 0)
    ret[rows_of(me), :] = outb[rows_of(me), :]

    weights = weight_ref[...].T
    for p, (low, high) in enumerate(pieces):
        amount((ep - 1) * (high - low), crecv.at[p]).wait()
        first, last = low // capacity, high // capacity

        def take_in(g, carry, low=low, high=high, first=first, last=last):
            for s in range(per_group):
                wide[g, s * chunk + low : s * chunk + high, :] = ret[
                    rows_of(g * per_group + s, low, high - low), :
                ].astype(F32)
            gather_up(g, first, last)
            return carry

        lax.fori_loop(0, GROUPS, take_in, 0)
        cols = slice(first * LANES, last * LANES)
        chosen = xs[:, cols]
        total = weights[:, 0:1] * dot(picks[0], chosen)
        total = total + weights[:, 1:2] * dot(picks[1], chosen)
        moe_out[:, cols] = total.astype(BF16)
        if p == len(pieces) - 2:
            for k in range(1, tp):
                mix_copy(k).wait()
            summed = mixr[0].astype(F32)
            for part in range(1, tp):
                summed = summed + mixr[part].astype(F32)
            mix_out[...] = rms_scale(summed, mix_gain_ref[...]).astype(BF16)

    amount((ep - 1) * chunk, dsend).wait()
    amount((ep - 1) * chunk, csend).wait()
    for k in range(1, planes):

        @pl.when(my_z + k < planes)
        def _(k=k):
            z_copy(k).wait_send()

    def wait_kv(j, carry):
        c_copy(0, j).wait_send()
        for k in range(1, columns):
            x_copy(k, j).wait_send()
            c_copy(k, j).wait_send()
        return carry

    lax.fori_loop(0, my_z + 1, wait_kv, 0)
    for i in range(len(stages)):
        for way in (0, 1):
            near(i, way).wait_send()
            far(i, way).wait_send()


def body(
    planes,
    columns,
    queries,
    keys_values,
    log_gate_cum,
    mix_weight,
    mix_gain,
    moe_in,
    moe_gain,
    routes,
    route_weight,
    expert_gate,
    expert_up,
    expert_down,
):
    ep = planes * columns * 2
    tp = 4
    tokens, model = moe_in.shape
    tiles = model // LANES
    capacity = 3 * routes.shape[1] * tokens // (2 * ep)
    slots = ep * capacity
    rows = queries.shape[0]
    heads = queries.shape[1] // HEAD
    depth, width = expert_gate.shape[1:]
    stages = 1 + len(PIECES)
    vmem = pl.BlockSpec(memory_space=pltpu.VMEM)
    hbm = pl.BlockSpec(memory_space=pl.ANY)
    dma = pltpu.SemaphoreType.DMA
    return pl.pallas_call(
        functools.partial(step_kernel, planes, columns),
        out_shape=(
            jax.ShapeDtypeStruct((rows // tp, model), BF16),
            jax.ShapeDtypeStruct((tokens, model), BF16),
        ),
        in_specs=[hbm] * 4 + [vmem, hbm, vmem, vmem, vmem] + [hbm] * 3,
        out_specs=(vmem, vmem),
        scratch_shapes=[
            pltpu.VMEM((tokens, model), BF16),
            pltpu.VMEM(queries.shape, BF16),
            pltpu.VMEM(log_gate_cum.shape, F32),
            pltpu.VMEM(mix_weight.shape, BF16),
            pltpu.VMEM((tp, depth, width), BF16),
            pltpu.VMEM((tp, depth, width), BF16),
            pltpu.VMEM((tp, width, model), BF16),
            pltpu.VMEM((ep, rows, 2 * HEAD), BF16),
            pltpu.VMEM((2, tokens, slots), BF16),
            pltpu.VMEM((slots * tiles, LANES), BF16),
            pltpu.VMEM((slots * tiles, LANES), BF16),
            pltpu.VMEM((slots, model), BF16),
            pltpu.VMEM((tp, slots, width), BF16),
            pltpu.VMEM((GROUPS, slots * tiles // GROUPS, LANES), F32),
            pltpu.VMEM((slots * tiles, LANES), BF16),
            pltpu.VMEM((slots * tiles, LANES), BF16),
            pltpu.VMEM((heads * rows, 2 * HEAD), BF16),
            pltpu.VMEM((heads, rows, LANES), F32),
            pltpu.VMEM((heads, rows, LANES), F32),
            pltpu.VMEM((heads, rows, LANES), F32),
            pltpu.VMEM((rows, model), BF16),
            pltpu.VMEM((tp, rows // tp, model), BF16),
            dma((8,)),
            dma((stages, tp)),
            dma((stages, tp)),
            dma((planes,)),
            dma((planes,)),
            dma((columns * planes,)),
            dma((columns * planes,)),
            dma((columns * planes,)),
            dma((columns * planes,)),
            dma,
            dma((GROUPS,)),
            dma,
            dma((len(PIECES) - 1,)),
            dma((tp,)),
            dma((tp,)),
        ],
        compiler_params=pltpu.CompilerParams(
            collective_id=0, has_side_effects=True, vmem_limit_bytes=64000 * 1024
        ),
        name="layer_step",
    )(
        queries,
        keys_values,
        log_gate_cum,
        mix_weight,
        mix_gain[None],
        moe_in,
        moe_gain[None],
        routes.T,
        route_weight.T,
        expert_gate[0],
        expert_up[0],
        expert_down[0],
    )


def solution(mesh, planes=8, columns=4):
    in_specs = (
        P("ep", "tp"),
        P("ep", "tp"),
        P("tp", None),
        P("tp", None),
        P(),
        P(("ep", "tp"), None),
        P(),
        P(("ep", "tp"), None),
        P(("ep", "tp"), None),
        P("ep", None, "tp"),
        P("ep", None, "tp"),
        P("ep", "tp", None),
    )
    out_specs = (P(("ep", "tp"), None), P(("ep", "tp"), None))
    return jax.shard_map(
        functools.partial(body, planes, columns),
        mesh=mesh,
        in_specs=in_specs,
        out_specs=out_specs,
        check_vma=False,
    )
```

```python
import functools

import jax
import jax.numpy as jnp
from jax import lax
from jax.experimental import pallas as pl
from jax.experimental.pallas import tpu as pltpu
from jax.sharding import PartitionSpec as P

HEAD = 64
EPSILON = 1e-06
NEGATIVE = -3e38
LANES = 128
KEY_BLOCK = 512
GROUPS = 4
STORES = 3
PIECES = (0, 32, 64, 96, 128, 144)
MESH = pl.DeviceIdType.MESH
F32 = jnp.float32
BF16 = jnp.bfloat16


def dot(a, b):
    return jnp.dot(a, b, preferred_element_type=F32)


def rms_scale(values, gain):
    return values * lax.rsqrt(jnp.mean(values * values, axis=-1, keepdims=True) + EPSILON) * gain


def step_kernel(
    planes,
    columns,
    q_hbm,
    kv_hbm,
    gate_log_hbm,
    mixw_hbm,
    mix_gain_ref,
    x_hbm,
    moe_gain_ref,
    routes_ref,
    weight_ref,
    gate_hbm,
    up_hbm,
    down_hbm,
    mix_out,
    moe_out,
    x_ref,
    q_ref,
    gate_log_ref,
    mixw_ref,
    wg,
    wu,
    wd,
    kvb,
    picks,
    send,
    recv,
    xs,
    hid,
    wide,
    outb,
    ret,
    qs,
    m_ref,
    l_ref,
    acc_ref,
    mixb,
    mixr,
    own_sem,
    wsend,
    wrecv,
    kzsend,
    kzrecv,
    kxsend,
    kxrecv,
    kcsend,
    kcrecv,
    dsend,
    drecv,
    csend,
    crecv,
    msend,
    mrecv,
):
    ep = planes * columns * 2
    tp = 4
    me = lax.axis_index("ep")
    my = lax.axis_index("tp")
    my_z = me // (2 * columns)
    my_x = (me // 2) % columns
    my_c = me % 2
    tokens, model = x_ref.shape
    tiles = model // LANES
    slots = xs.shape[0]
    capacity = slots // ep
    chunk = capacity * tiles
    per_group = ep // GROUPS
    group_rows = slots // GROUPS
    my_group = me // per_group
    queries = q_ref.shape[0]
    heads = q_ref.shape[1] // HEAD

    def at(e, t=None):
        return {"ep": e, "tp": my if t is None else t}

    def remote(src, dst, s_sem, r_sem, where):
        return pltpu.make_async_remote_copy(
            src_ref=src,
            dst_ref=dst,
            send_sem=s_sem,
            recv_sem=r_sem,
            device_id=where,
            device_id_type=MESH,
        )

    barrier = pltpu.get_barrier_semaphore()

    def greet_ep(k, carry):
        pl.semaphore_signal(barrier, inc=1, device_id=at((me + k) % ep), device_id_type=MESH)
        return carry

    lax.fori_loop(1, ep, greet_ep, 0)
    for k in range(1, tp):
        pl.semaphore_signal(barrier, inc=1, device_id=at(me, (my + k) % tp), device_id_type=MESH)

    own = [
        pltpu.make_async_copy(src, dst, own_sem.at[i])
        for i, (src, dst) in enumerate(
            (
                (x_hbm, x_ref),
                (kv_hbm, kvb.at[me]),
                (q_hbm, q_ref),
                (gate_log_hbm, gate_log_ref),
                (mixw_hbm, mixw_ref),
                (gate_hbm, wg.at[my]),
                (up_hbm, wu.at[my]),
                (down_hbm, wd.at[my]),
            )
        )
    ]
    for copy in own:
        copy.start()

    ids = lax.broadcasted_iota(jnp.int32, (tokens, ep), 1)
    lower = (
        lax.broadcasted_iota(jnp.int32, (tokens, tokens), 1)
        < lax.broadcasted_iota(jnp.int32, (tokens, tokens), 0)
    ).astype(BF16)
    slot_ids = lax.broadcasted_iota(jnp.int32, (tokens, slots), 1)
    taken = jnp.zeros((1, ep), F32)
    routes = routes_ref[...].T
    for side in range(2):
        expert = routes[:, side : side + 1]
        named = (ids == expert).astype(F32)
        before = dot(lower, named.astype(BF16)) + taken
        taken = taken + jnp.sum(named, axis=0, keepdims=True)
        position = jnp.sum(named * before, axis=1, keepdims=True).astype(jnp.int32)
        slot = (expert // per_group) * group_rows + position * per_group + expert % per_group
        picks[side] = jnp.where(slot_ids == slot, 1.0, 0.0).astype(BF16)

    pl.semaphore_wait(barrier, ep - 1 + tp - 1)

    ends = [-(-b // capacity) * LANES for b in PIECES]
    stages = [(gate_hbm, wg, None), (up_hbm, wu, None)] + [
        (down_hbm, wd, pl.ds(a, b - a)) for a, b in zip(ends[:-1], ends[1:])
    ]

    def part_of(i, source, half=None):
        src, dst, cols = stages[i]
        if half is None:
            return (src, dst.at[source]) if cols is None else (
                src.at[:, cols], dst.at[source, :, cols]
            )
        size = dst.shape[1] // 2
        band = pl.ds(half * size, size)
        block = dst.at[source, band] if cols is None else dst.at[source, band, cols]
        return block, block

    def near(i, way):
        src, dst = part_of(i, my)
        peer = (my + (1, 3)[way]) % tp
        return remote(src, dst, wsend.at[i, way], wrecv.at[i, way], at(me, peer))

    def far(i, way):
        src, dst = part_of(i, (my + (3, 1)[way]) % tp, way)
        peer = (my + (1, 3)[way]) % tp
        return remote(src, dst, wsend.at[i, 2 + way], wrecv.at[i, 2 + way], at(me, peer))

    def start_near(i):
        for way in (0, 1):
            near(i, way).start()

    def relay(i):
        for way in (0, 1):
            near(i, way).wait_recv()
            far(i, way).start()

    start_near(0)
    start_near(1)

    def kv_slot(z, x, c):
        return (z * columns + x) * 2 + c

    def z_copy(k):
        return remote(
            kv_hbm,
            kvb.at[me],
            kzsend.at[k],
            kzrecv.at[k],
            at(kv_slot((my_z + k) % planes, my_x, my_c)),
        )

    for k in range(1, planes):

        @pl.when(my_z + k < planes)
        def _(k=k):
            z_copy(k).start()

    own[0].wait()
    normed = rms_scale(x_ref[...].astype(F32), moe_gain_ref[...]).astype(BF16)
    both = picks[0] + picks[1]

    def lay_out(g, value, first):
        for j in range(value.shape[1] // LANES):
            for r in range(capacity):
                wide[g, pl.ds((first + j) * capacity + r, per_group, stride=chunk), :] = value[
                    r * per_group : (r + 1) * per_group, j * LANES : (j + 1) * LANES
                ]

    def gather_up(g, first, last):
        rows = pl.multiple_of(g * group_rows, 16)
        for j in range(first, last):
            for r in range(capacity):
                xs[pl.ds(rows + r * per_group, per_group), j * LANES : (j + 1) * LANES] = wide[
                    g, pl.ds(j * capacity + r, per_group, stride=chunk), :
                ].astype(BF16)

    for pair in range(tiles // 2):
        moved = lax.dot_general(
            both,
            normed[:, pair * 2 * LANES : (pair + 1) * 2 * LANES],
            (((0,), (0,)), ((), ())),
            preferred_element_type=F32,
        )
        for g in range(GROUPS):
            lay_out(g, moved[g * group_rows : (g + 1) * group_rows], 2 * pair)
    for g in range(GROUPS):
        send[g * per_group * chunk : (g + 1) * per_group * chunk, :] = wide[g].astype(BF16)

    def rows_of(e, start=0, size=chunk):
        return pl.ds(pl.multiple_of(e * chunk + start, 16), size)

    def start_dispatch(k, carry):
        e = (me + 1 + (k + ep // 3) % (ep - 1)) % ep
        remote(
            send.at[rows_of(e)], recv.at[rows_of(me)], dsend, drecv.at[my_group], at(e)
        ).start()
        return carry

    lax.fori_loop(1, ep, start_dispatch, 0)
    recv[rows_of(me), :] = send[rows_of(me), :]

    def amount(rows, sem):
        return pltpu.make_async_copy(send.at[pl.ds(0, rows)], recv.at[pl.ds(0, rows)], sem)

    for i in (1, 2, 3):
        own[i].wait()
    for h in range(heads):
        part = q_ref[:, h * HEAD : (h + 1) * HEAD].astype(F32) * HEAD ** (-0.5)
        qs[h * queries : (h + 1) * queries, :] = jnp.concatenate(
            [part, jnp.zeros_like(part)], axis=1
        ).astype(BF16)
        m_ref[h] = jnp.full((queries, LANES), NEGATIVE, F32)
        l_ref[h] = jnp.zeros((queries, LANES), F32)
        acc_ref[h] = jnp.zeros((queries, LANES), F32)

    def x_copy(k, j):
        slab = kvb.at[kv_slot((my_z + planes - j) % planes, my_x, my_c)]
        return remote(
            slab,
            slab,
            kxsend.at[k * planes + j],
            kxrecv.at[k * planes + j],
            at(kv_slot(my_z, (my_x + k) % columns, my_c)),
        )

    def c_copy(k, j):
        slab = kvb.at[kv_slot((my_z + planes - j) % planes, (my_x + columns - k) % columns, my_c)]
        return remote(
            slab, slab, kcsend.at[k * planes + j], kcrecv.at[k * planes + j], at(me + 1 - 2 * my_c)
        )

    base = gate_log_ref[:, pl.ds(pl.multiple_of(me * queries, LANES), LANES)][:, 0:1]
    slabs = KEY_BLOCK // queries

    def attend(i, masked):
        keys = kvb[pl.ds(i * slabs, slabs)].reshape(KEY_BLOCK, 2 * HEAD)
        start = pl.multiple_of(i * KEY_BLOCK, KEY_BLOCK)
        bias = base - gate_log_ref[:, pl.ds(start, KEY_BLOCK)]
        scores = lax.dot_general(
            qs[...], keys, (((1,), (1,)), ((), ())), preferred_element_type=F32
        )
        weights = []
        factors = []
        for h in range(heads):
            part = scores[h * queries : (h + 1) * queries] + bias[h : h + 1, :]
            if masked:
                key_pos = start + lax.broadcasted_iota(jnp.int32, part.shape, 1)
                query_pos = me * queries + lax.broadcasted_iota(jnp.int32, part.shape, 0)
                part = jnp.where(key_pos <= query_pos, part, NEGATIVE)
            old = m_ref[h]
            new = jnp.maximum(old, jnp.max(part, axis=1, keepdims=True))
            factor = jnp.exp(old - new)
            weight = jnp.exp(part - jnp.concatenate([new] * (KEY_BLOCK // LANES), axis=1))
            summed = weight[:, :LANES]
            for t in range(1, KEY_BLOCK // LANES):
                summed = summed + weight[:, t * LANES : (t + 1) * LANES]
            m_ref[h] = new
            l_ref[h] = l_ref[h] * factor + summed
            weights.append(weight.astype(BF16))
            factors.append(factor)
        moved = dot(jnp.concatenate(weights, axis=0), keys)
        for h in range(heads):
            acc_ref[h] = acc_ref[h] * factors[h] + moved[h * queries : (h + 1) * queries]

    def attend_step(t, carry):
        @pl.when(t <= my_z)
        def _():
            @pl.when(t > 0)
            def _():
                z_copy(t).wait_recv()

            for k in range(1, columns):
                x_copy(k, t).start()
            c_copy(0, t).start()

        @pl.when((t >= 1) & (t <= my_z + 1))
        def _():
            for k in range(1, columns):
                x_copy(k, t - 1).wait_recv()
                c_copy(k, t - 1).start()

        @pl.when(t == planes // 2 + 1)
        def _():
            relay(0)
            start_near(2)

        @pl.when(t >= 2)
        def _():
            for k in range(columns):
                c_copy(k, t - 2).wait_recv()
            first = (my_z + 2 - t) * columns

            def whole(i, carry):
                attend(i, False)
                return carry

            lax.fori_loop(first, first + jnp.where(t == 2, my_x, columns), whole, 0)

            @pl.when(t == 2)
            def _():
                attend(me // slabs, True)

        return carry

    lax.fori_loop(0, my_z + 3, attend_step, 0)

    @pl.when(my_z + 2 < planes // 2 + 1)
    def _():
        relay(0)
        start_near(2)

    relay(1)

    own[4].wait()
    attended = jnp.concatenate(
        [acc_ref[h][:, HEAD:] / jnp.sum(l_ref[h], axis=1, keepdims=True) for h in range(heads)],
        axis=1,
    ).astype(BF16)
    mixb[...] = dot(attended, mixw_ref[...]).astype(BF16)
    share = queries // tp

    def mix_copy(k):
        t = (my + k) % tp
        return remote(
            mixb.at[pl.ds(pl.multiple_of(t * share, 16), share)],
            mixr.at[k],
            msend.at[k],
            mrecv.at[k],
            at(me, t),
        )

    mixr[0] = mixb[pl.ds(pl.multiple_of(my * share, 16), share), :]

    for i in (5, 6, 7):
        own[i].wait()
    for g in range(GROUPS):

        @pl.when(g == my_group)
        def _(g=g):
            amount((per_group - 1) * chunk, drecv.at[g]).wait()

        @pl.when(g != my_group)
        def _(g=g):
            amount(per_group * chunk, drecv.at[g]).wait()

    def spread(g, carry):
        size = per_group * chunk
        wide[g] = recv[pl.ds(pl.multiple_of(g * size, 16), size), :].astype(F32)
        gather_up(g, 0, tiles)
        return carry

    lax.fori_loop(0, GROUPS, spread, 0)

    def expand(k, carry):
        q = (my + k) % tp
        up_part = dot(xs[...], wu[q])
        gate_part = dot(xs[...], wg[q])
        hid[q] = (gate_part / (1.0 + jnp.exp(-gate_part)) * up_part).astype(BF16)
        return carry

    def expand_step(i, carry):
        @pl.when(i == 3)
        def _():
            relay(2)
            for m in range(3, min(5, len(stages))):
                start_near(m)
            for m in (0, 1):
                for way in (0, 1):
                    far(m, way).wait_recv()

        return expand(i + (i // 2) * (5 - 2 * i), carry)

    lax.fori_loop(0, tp, expand_step, 0)

    pieces = list(zip(PIECES[:-1], PIECES[1:]))

    def contract(p, i):
        low, high = pieces[p]
        g = (i + my_group + GROUPS // 2) % GROUPS
        rows = pl.ds(pl.multiple_of(g * group_rows, 16), group_rows)
        first, last = ends[p], ends[p + 1]
        total = jnp.zeros((group_rows, last - first), F32)
        for q in range(tp):
            total = total + dot(hid[q, rows, :], wd[q, :, first:last])
        lay_out(g, total, first // LANES)
        for s in range(per_group):
            outb[rows_of(g * per_group + s, low, high - low), :] = wide[
                g, s * chunk + low : s * chunk + high, :
            ].astype(BF16)

        def start_combine(j, carry):
            s = g * per_group + (j + me) % per_group

            @pl.when(s != me)
            def _():
                remote(
                    outb.at[rows_of(s, low, high - low)],
                    ret.at[rows_of(me, low, high - low)],
                    csend,
                    crecv.at[p],
                    at(s),
                ).start()

            return carry

        lax.fori_loop(0, per_group, start_combine, 0)

    for p in range(len(pieces)):
        if p > 0:
            relay(2 + p)
            if p + 2 < len(pieces):
                start_near(4 + p)
        if p == len(pieces) - 1:
            for k in range(1, tp):
                mix_copy(k).start()
        for way in (0, 1):
            far(2 + p, way).wait_recv()

        def contract_step(i, carry, p=p):
            contract(p, i)
            return carry

        lax.fori_loop(0, GROUPS, contract_step, 0)
    ret[rows_of(me), :] = outb[rows_of(me), :]

    weights = weight_ref[...].T
    for p, (low, high) in enumerate(pieces):
        amount((ep - 1) * (high - low), crecv.at[p]).wait()
        first, last = low // capacity, high // capacity

        def take_in(g, carry, low=low, high=high, first=first, last=last):
            for s in range(per_group):
                wide[g, s * chunk + low : s * chunk + high, :] = ret[
                    rows_of(g * per_group + s, low, high - low), :
                ].astype(F32)
            gather_up(g, first, last)
            return carry

        lax.fori_loop(0, GROUPS, take_in, 0)
        cols = slice(first * LANES, last * LANES)
        chosen = xs[:, cols]
        total = weights[:, 0:1] * dot(picks[0], chosen)
        total = total + weights[:, 1:2] * dot(picks[1], chosen)
        moe_out[:, cols] = total.astype(BF16)
        if p == len(pieces) - 2:
            for k in range(1, tp):
                mix_copy(k).wait()
            summed = mixr[0].astype(F32)
            for part in range(1, tp):
                summed = summed + mixr[part].astype(F32)
            mix_out[...] = rms_scale(summed, mix_gain_ref[...]).astype(BF16)

    amount((ep - 1) * chunk, dsend).wait()
    amount((ep - 1) * chunk, csend).wait()
    for k in range(1, planes):

        @pl.when(my_z + k < planes)
        def _(k=k):
            z_copy(k).wait_send()

    def wait_kv(j, carry):
        c_copy(0, j).wait_send()
        for k in range(1, columns):
            x_copy(k, j).wait_send()
            c_copy(k, j).wait_send()
        return carry

    lax.fori_loop(0, my_z + 1, wait_kv, 0)
    for i in range(len(stages)):
        for way in (0, 1):
            near(i, way).wait_send()
            far(i, way).wait_send()


def store_kernel(mixed_in, experts_in, mixed_out, experts_out, mixed, experts, load_sem, save_sem):
    band = experts.shape[0] // STORES
    bands = [pl.ds(i * band, band) for i in range(STORES)]
    views = [(experts_in.at[b], experts.at[b], experts_out.at[b]) for b in bands]
    views.append((mixed_in, mixed, mixed_out))
    loads = [
        pltpu.make_async_copy(src, mid, load_sem.at[i]) for i, (src, mid, _) in enumerate(views)
    ]
    saves = [
        pltpu.make_async_copy(mid, dst, save_sem.at[i]) for i, (_, mid, dst) in enumerate(views)
    ]
    for load in loads:
        load.start()
    for load, save in zip(loads, saves):
        load.wait()
        save.start()
    for save in saves:
        save.wait()


def body(
    planes,
    columns,
    queries,
    keys_values,
    log_gate_cum,
    mix_weight,
    mix_gain,
    moe_in,
    moe_gain,
    routes,
    route_weight,
    expert_gate,
    expert_up,
    expert_down,
):
    ep = planes * columns * 2
    tp = 4
    tokens, model = moe_in.shape
    tiles = model // LANES
    capacity = 3 * routes.shape[1] * tokens // (2 * ep)
    slots = ep * capacity
    rows = queries.shape[0]
    heads = queries.shape[1] // HEAD
    depth, width = expert_gate.shape[1:]
    stages = 1 + len(PIECES)
    vmem = pl.BlockSpec(memory_space=pltpu.VMEM)
    hbm = pl.BlockSpec(memory_space=pl.ANY)
    dma = pltpu.SemaphoreType.DMA
    mixed, experts = pl.pallas_call(
        functools.partial(step_kernel, planes, columns),
        out_shape=(
            jax.ShapeDtypeStruct((rows // tp, model), BF16),
            jax.ShapeDtypeStruct((tokens, model), BF16),
        ),
        in_specs=[hbm] * 4 + [vmem, hbm, vmem, vmem, vmem] + [hbm] * 3,
        out_specs=(vmem, vmem),
        scratch_shapes=[
            pltpu.VMEM((tokens, model), BF16),
            pltpu.VMEM(queries.shape, BF16),
            pltpu.VMEM(log_gate_cum.shape, F32),
            pltpu.VMEM(mix_weight.shape, BF16),
            pltpu.VMEM((tp, depth, width), BF16),
            pltpu.VMEM((tp, depth, width), BF16),
            pltpu.VMEM((tp, width, model), BF16),
            pltpu.VMEM((ep, rows, 2 * HEAD), BF16),
            pltpu.VMEM((2, tokens, slots), BF16),
            pltpu.VMEM((slots * tiles, LANES), BF16),
            pltpu.VMEM((slots * tiles, LANES), BF16),
            pltpu.VMEM((slots, model), BF16),
            pltpu.VMEM((tp, slots, width), BF16),
            pltpu.VMEM((GROUPS, slots * tiles // GROUPS, LANES), F32),
            pltpu.VMEM((slots * tiles, LANES), BF16),
            pltpu.VMEM((slots * tiles, LANES), BF16),
            pltpu.VMEM((heads * rows, 2 * HEAD), BF16),
            pltpu.VMEM((heads, rows, LANES), F32),
            pltpu.VMEM((heads, rows, LANES), F32),
            pltpu.VMEM((heads, rows, LANES), F32),
            pltpu.VMEM((rows, model), BF16),
            pltpu.VMEM((tp, rows // tp, model), BF16),
            dma((8,)),
            dma((stages, tp)),
            dma((stages, tp)),
            dma((planes,)),
            dma((planes,)),
            dma((columns * planes,)),
            dma((columns * planes,)),
            dma((columns * planes,)),
            dma((columns * planes,)),
            dma,
            dma((GROUPS,)),
            dma,
            dma((len(PIECES) - 1,)),
            dma((tp,)),
            dma((tp,)),
        ],
        compiler_params=pltpu.CompilerParams(
            collective_id=0, has_side_effects=True, vmem_limit_bytes=64000 * 1024
        ),
        name="layer_step",
    )(
        queries,
        keys_values,
        log_gate_cum,
        mix_weight,
        mix_gain[None],
        moe_in,
        moe_gain[None],
        routes.T,
        route_weight.T,
        expert_gate[0],
        expert_up[0],
        expert_down[0],
    )

    outs = (
        jax.ShapeDtypeStruct(mixed.shape, BF16),
        jax.ShapeDtypeStruct(experts.shape, BF16),
    )
    return pl.pallas_call(
        store_kernel,
        out_shape=outs,
        in_specs=[hbm, hbm],
        out_specs=(hbm, hbm),
        scratch_shapes=[
            pltpu.VMEM(mixed.shape, BF16),
            pltpu.VMEM(experts.shape, BF16),
            dma((1 + STORES,)),
            dma((1 + STORES,)),
        ],
        compiler_params=pltpu.CompilerParams(vmem_limit_bytes=64000 * 1024),
        name="store",
    )(mixed, experts)


def solution(mesh, planes=8, columns=4):
    in_specs = (
        P("ep", "tp"),
        P("ep", "tp"),
        P("tp", None),
        P("tp", None),
        P(),
        P(("ep", "tp"), None),
        P(),
        P(("ep", "tp"), None),
        P(("ep", "tp"), None),
        P("ep", None, "tp"),
        P("ep", None, "tp"),
        P("ep", "tp", None),
    )
    out_specs = (P(("ep", "tp"), None), P(("ep", "tp"), None))
    return jax.shard_map(
        functools.partial(body, planes, columns),
        mesh=mesh,
        in_specs=in_specs,
        out_specs=out_specs,
        check_vma=False,
    )
```
